32 devices in a mesh: kv: 8 (over z, x), tp: 4 (over y, core).
Axes of the slice: x: 2, y: 2, z: 4, core: 2. Of those that a mesh axis runs over, the one named last changes fastest.
Arguments:
- layer_input: bfloat16 [256, 4096], P('tp', 'kv'), may hold values from -6 to 6
- seq_lengths: int32 [64], P('kv'), may hold values from 1 to 4, 112 in all
- delta_state: float32 [64, 16, 128, 128], P('kv', 'tp'), may hold values from -0.4 to 0.4
- attn_gain: bfloat16 [4096], replicated, may hold values from 0.099609375 to 1.8984375
- w_query: bfloat16 [4096, 2048], P('kv', 'tp'), may hold values from -0.09375 to 0.09375
- w_key: bfloat16 [4096, 2048], P('kv', 'tp'), may hold values from -0.09375 to 0.09375
- w_value: bfloat16 [4096, 2048], P('kv', 'tp'), may hold values from -0.09375 to 0.09375
- w_outgate: bfloat16 [4096, 2048], P('kv', 'tp'), may hold values from -0.09375 to 0.09375
- w_write: bfloat16 [4096, 16], P('kv', 'tp'), may hold values from -0.09375 to 0.09375
- w_forget: bfloat16 [4096, 16], P('kv', 'tp'), may hold values from -0.09375 to 0.09375
- forget_rate: float32 [16], P('tp'), may hold values from 0.02 to 2
- head_gain: float32 [128], replicated, may hold values from 0.1 to 1.9
- w_out: bfloat16 [2048, 4096], P('tp', 'kv'), may hold values from -0.125 to 0.125
- mixer_gain: bfloat16 [4096], replicated, may hold values from 0.099609375 to 1.8984375
- w_gate: bfloat16 [4096, 11264], P('kv', 'tp'), may hold values from -0.09375 to 0.09375
- w_up: bfloat16 [4096, 11264], P('kv', 'tp'), may hold values from -0.09375 to 0.09375
- w_down: bfloat16 [11264, 4096], P('tp', 'kv'), may hold values from -0.0546875 to 0.0546875
Outputs:
- layer_output: bfloat16 [256, 4096], P('tp', 'kv')
- next_state: float32 [64, 16, 128, 128], P('kv', 'tp')
The draws below stay inside these ranges and needn't reach their ends.
Inputs may be any that keep to these rules, and one draw needn't show every extreme that they name: `seq_lengths`: the lengths add up to 112.
All inputs are finite; a program needn't handle non-finite values. No bound on the sum of `seq_lengths` on one device may be relied on, other than what follows from the above.
Results may differ from the reference program's by a relative error of at most 0.024.
Values may be sent and summed in bfloat16 or wider, within the bound.
No kernel may reach another device: no remote copies, remote signals or barrier semaphores. Data moves between devices by JAX's collectives and lax.ppermute only.
A program may use at most 64 MiB of HBM per device.

```python
import math
import jax
import jax.numpy as jnp
import numpy as np
from jax import lax

D = 4096
H = 16
DK = 128
FF = 11264
NEW = 4
SEQS = 64
ROWS = 256
HW = 2048
N_TP = 4


def steps_of(stream_key, dims, split, low, largest):
    def one(axis_at, blocks):
        steps = jax.random.uniform(jax.random.fold_in(jax.random.fold_in(stream_key, 6), axis_at), (blocks,), jnp.float32, low / len(split), largest / len(split))
        return jnp.repeat(jnp.exp(steps), dims[axis_at] // blocks).reshape((-1,) + (1,) * (len(dims) - axis_at - 1))

    loudness = one(*split[0])
    for cut in split[1:]:
        loudness = loudness * one(*cut)
    return loudness


def length_profile(count, total, bound, slope):
    weights = [(1 << 20) // math.isqrt(rank ** slope) + 1 for rank in range(2, count + 1)]
    surplus, counts = total - bound - (count - 1), [1] * (count - 1)
    while surplus > 0:
        candidates = [i for i in range(count - 1) if counts[i] < bound]
        whole, remaining = sum([weights[i] for i in candidates]), surplus
        for i in candidates:
            extra = min(bound - counts[i], max(1, remaining * weights[i] // whole), surplus)
            counts[i] = counts[i] + extra
            surplus = surplus - extra
    return np.array([bound] + counts)


def ragged(rng, amount, total, bound, lean):
    if amount == 2:
        one = jax.random.randint(rng, (), max(1, total - bound), min(bound, total - 1) + 1)
        return jnp.stack([one, total - one])
    sizes = jnp.asarray(length_profile(amount, total, bound, lean), jnp.int32)
    twos = (amount - 1) // 2
    source_of, taker = sizes[1:1 + 2 * twos:2], sizes[2:2 + 2 * twos:2]
    room = jnp.minimum(source_of - 1, bound - taker)
    moved = jax.random.randint(jax.random.fold_in(rng, 1), (twos,), 0, 1 << 20) % (room + 1)
    sizes = sizes.at[1:1 + 2 * twos:2].set(source_of - moved).at[2:2 + 2 * twos:2].set(taker + moved)
    return sizes[jax.random.permutation(jax.random.fold_in(rng, 2), amount)]


def bell_draw(rng, extent, spread, most, pieces=(), held_as=jnp.bfloat16):
    level = steps_of(rng, extent, pieces, -0.22, 0.18) if pieces else 1.0
    array = jax.random.normal(rng, extent, jnp.float32) * spread * level
    return jnp.minimum(jnp.maximum(array, -most), most).astype(held_as)


def setup_inputs(seed: int = 0) -> dict:
    key_of = jax.random.split(jax.random.key(seed), 18)
    layer_input = bell_draw(key_of[0], (ROWS, D), 1.0, 6.0, ((0, 4), (1, 8)))
    seq_lengths = ragged(key_of[1], SEQS, SEQS + 3 * SEQS // 4, NEW, 2).astype(jnp.int32)
    delta_state = bell_draw(key_of[2], (SEQS, H, DK, DK), 0.05, 0.4, ((0, 8), (1, 4)), jnp.float32)
    attn_gain = jnp.clip(1.0 + 0.18 * jax.random.normal(key_of[3], (D,), jnp.float32), 0.099609375, 1.8984375).astype(jnp.bfloat16)
    w_query = bell_draw(key_of[4], (D, HW), D ** -0.5, 0.09375, ((0, 8), (1, 4)))
    w_key = bell_draw(key_of[5], (D, HW), D ** -0.5, 0.09375, ((0, 8), (1, 4)))
    w_value = bell_draw(key_of[6], (D, HW), D ** -0.5, 0.09375, ((0, 8), (1, 4)))
    w_outgate = bell_draw(key_of[7], (D, HW), D ** -0.5, 0.09375, ((0, 8), (1, 4)))
    w_write = bell_draw(key_of[8], (D, H), D ** -0.5, 0.09375, ((0, 8), (1, 4)))
    w_forget = bell_draw(key_of[9], (D, H), D ** -0.5, 0.09375, ((0, 8), (1, 4)))
    forget_rate = jnp.clip(jnp.exp(math.log(2.0) - 4.6051702 * jax.random.uniform(key_of[10], (H,), jnp.float32) ** steps_of(key_of[10], (H,), ((0, 4),), -0.2, 0.2)), 0.02, 2.0)
    head_gain = jnp.clip(1.0 + 0.18 * jax.random.normal(key_of[11], (DK,), jnp.float32), 0.1, 1.9)
    w_out = bell_draw(key_of[12], (HW, D), HW ** -0.5, 0.125, ((0, 4), (1, 8)))
    mixer_gain = jnp.clip(1.0 + 0.18 * jax.random.normal(key_of[13], (D,), jnp.float32), 0.099609375, 1.8984375).astype(jnp.bfloat16)
    w_gate = bell_draw(key_of[14], (D, FF), D ** -0.5, 0.09375, ((0, 8), (1, 4)))
    w_up = bell_draw(key_of[15], (D, FF), D ** -0.5, 0.09375, ((0, 8), (1, 4)))
    w_down = bell_draw(key_of[16], (FF, D), FF ** -0.5, 0.0546875, ((0, 4), (1, 8)))
    return dict(layer_input=layer_input, seq_lengths=seq_lengths, delta_state=delta_state, attn_gain=attn_gain, w_query=w_query, w_key=w_key, w_value=w_value, w_outgate=w_outgate, w_write=w_write, w_forget=w_forget, forget_rate=forget_rate, head_gain=head_gain, w_out=w_out, mixer_gain=mixer_gain, w_gate=w_gate, w_up=w_up, w_down=w_down)


EPS = 1e-06

def unit_norm(vectors):
    return vectors * lax.rsqrt(lax.optimization_barrier(jnp.sum(vectors * vectors, axis=-1, keepdims=True)) + EPS)

def run_delta(carried, query_unit, key_unit, value_act, write_rate, log_keep, live):
    readings = []
    for position in range(query_unit.shape[1]):
        active = live[:, position][:, None]
        beta = write_rate[:, position] * active
        keep = jnp.exp(log_keep[:, position] * active)
        key_now = key_unit[:, position]
        recalled = jnp.einsum('shk,shkv->shv', key_now, carried, precision=lax.Precision.HIGHEST)
        update = beta[:, :, None] * (value_act[:, position] - keep[:, :, None] * recalled)
        carried = keep[:, :, None, None] * carried + key_now[:, :, :, None] * update[:, :, None, :]
        reading = jnp.einsum('shk,shkv->shv', query_unit[:, position], carried, precision=lax.Precision.HIGHEST)
        readings.append(reading * active[:, :, None])
    return (carried, jnp.stack(readings, axis=1))

def reference(layer_input, seq_lengths, delta_state, attn_gain, w_query, w_key, w_value, w_outgate, w_write, w_forget, forget_rate, head_gain, w_out, mixer_gain, w_gate, w_up, w_down):
    rows_wide = layer_input.astype(jnp.float32)
    first_scale = lax.rsqrt(lax.optimization_barrier(jnp.mean(rows_wide * rows_wide, axis=1, keepdims=True)) + EPS)
    normed_in = (rows_wide * attn_gain.astype(jnp.float32)).astype(jnp.bfloat16)

    def project(weight):
        return first_scale * jnp.dot(normed_in, weight, preferred_element_type=jnp.float32)

    def split_heads(block):
        return block.reshape(SEQS, NEW, H, DK)
    query_unit = unit_norm(jax.nn.silu(split_heads(project(w_query)))) * DK ** (-0.5)
    key_unit = unit_norm(jax.nn.silu(split_heads(project(w_key))))
    value_act = jax.nn.silu(split_heads(project(w_value)))
    outgate = split_heads(project(w_outgate))
    write_rate = jax.nn.sigmoid(project(w_write).reshape(SEQS, NEW, H))
    log_keep = -forget_rate * jax.nn.softplus(project(w_forget).reshape(SEQS, NEW, H))
    positions = jnp.arange(NEW, dtype=jnp.int32)
    live = (positions[None, :] < seq_lengths[:, None]).astype(jnp.float32)
    carried, readings = run_delta(delta_state, query_unit, key_unit, value_act, write_rate, log_keep, live)
    normed = readings * lax.rsqrt(lax.optimization_barrier(jnp.mean(readings * readings, axis=-1, keepdims=True)) + EPS)
    normed = normed * head_gain * jax.nn.silu(outgate)
    mixed = normed.reshape(ROWS, HW).astype(jnp.bfloat16)
    grouped = mixed.reshape(ROWS, N_TP, HW // N_TP).astype(jnp.float32)
    out_groups = w_out.reshape(N_TP, HW // N_TP, D).astype(jnp.float32)
    group_terms = jnp.einsum('rgc,gcd->grd', grouped, out_groups)
    attended = lax.optimization_barrier(jnp.sum(group_terms.astype(jnp.bfloat16).astype(jnp.float32), axis=0))
    hidden_state = (rows_wide + attended).astype(jnp.bfloat16)
    hidden_wide = hidden_state.astype(jnp.float32)
    mixer_scale = lax.rsqrt(lax.optimization_barrier(jnp.mean(hidden_wide * hidden_wide, axis=1, keepdims=True)) + EPS)
    normed_mid = (hidden_wide * mixer_gain.astype(jnp.float32)).astype(jnp.bfloat16)
    gate_pre = mixer_scale * jnp.dot(normed_mid, w_gate, preferred_element_type=jnp.float32)
    up_pre = mixer_scale * jnp.dot(normed_mid, w_up, preferred_element_type=jnp.float32)
    activated = (jax.nn.silu(gate_pre) * up_pre).astype(jnp.bfloat16)
    mixer_out = jnp.dot(activated, w_down, preferred_element_type=jnp.float32)
    layer_output = (hidden_wide + mixer_out).astype(jnp.bfloat16)
    return (layer_output, carried)
```

```python
import functools

import jax
import jax.numpy as jnp
from jax import lax
from jax.experimental import pallas as pl
from jax.experimental.pallas import tpu as pltpu
from jax.sharding import PartitionSpec as P

D = 4096
NEW = 4
EPS = 1e-06
LANES = 128
HIGHEST = lax.Precision.HIGHEST


def swap(block, axis, distance):
    size = lax.axis_size(axis)
    return lax.ppermute(block, axis, [(i, i ^ distance) for i in range(size)])


def far_first(size):
    return sorted(range(1, size), key=lambda d: -d)


def block_of(rows, index, count):
    return lax.dynamic_slice_in_dim(rows, index * count, count)


def scatter_blocks(rows, axis):
    size, me = lax.axis_size(axis), lax.axis_index(axis)
    count = rows.shape[0] // size
    got = [swap(block_of(rows, me ^ d, count), axis, d) for d in far_first(size)]
    return [block_of(rows, me, count)] + got


def add_up(terms):
    total = terms[0].astype(jnp.float32)
    for term in terms[1:]:
        total = total + term.astype(jnp.float32)
    return total


def gather_blocks(block, axis):
    size = lax.axis_size(axis)
    return {0: block, **{d: swap(block, axis, d) for d in far_first(size)}}


def gathered_dot_kernel(distances, me_ref, *refs):
    blocks, (weight_ref, out_ref, rows_ref) = refs[: len(distances)], refs[len(distances) :]
    count = blocks[0].shape[0]
    me = me_ref[0]
    for distance, block in zip(distances, blocks):
        start = pl.multiple_of((me ^ distance) * count, count)
        rows_ref[pl.ds(start, count), :] = block[...]
    out_ref[...] = jnp.dot(
        rows_ref[...], weight_ref[...], preferred_element_type=jnp.float32
    ).astype(out_ref.dtype)


def gathered_dot(pieces, weight, axis):
    distances = tuple(pieces)
    count, depth = pieces[0].shape
    rows, width = count * len(distances), weight.shape[1]
    me = lax.axis_index(axis).astype(jnp.int32).reshape(1)
    in_vmem = pl.BlockSpec(memory_space=pltpu.VMEM)
    return pl.pallas_call(
        functools.partial(gathered_dot_kernel, distances),
        out_shape=jax.ShapeDtypeStruct((rows, width), jnp.bfloat16),
        in_specs=[pl.BlockSpec(memory_space=pltpu.SMEM)] + [in_vmem] * (len(distances) + 1),
        out_specs=in_vmem,
        scratch_shapes=[pltpu.VMEM((rows, depth), jnp.bfloat16)],
        cost_estimate=pl.CostEstimate(
            flops=2 * rows * depth * width, bytes_accessed=2 * depth * width, transcendentals=0
        ),
    )(me, *[pieces[d] for d in distances], weight)


def unit_norm(vectors):
    return vectors * lax.rsqrt(jnp.sum(vectors * vectors, axis=-1, keepdims=True) + EPS)


def delta_kernel(heads, proj_ref, aux_ref, gain_ref, state_ref, mixed_ref, next_ref):
    size = state_ref.shape[-1]
    wide = heads * size
    gain = gain_ref[...]
    aux = aux_ref[0]
    active = aux[:, 2 * heads : 2 * heads + 1]
    for head in range(heads):
        query_pre, key_pre, value_pre, gate_pre = (
            proj_ref[0, :, part * wide + head * size : part * wide + (head + 1) * size]
            for part in range(4)
        )
        query = unit_norm(jax.nn.silu(query_pre)) * size ** (-0.5)
        key = unit_norm(jax.nn.silu(key_pre))
        value = jax.nn.silu(value_pre)
        state = state_ref[0, head]
        both = jnp.concatenate([key, query], axis=0)
        first = jnp.dot(both, state, precision=HIGHEST, preferred_element_type=jnp.float32)
        pair = lax.dot_general(
            both,
            key,
            (((1,), (1,)), ((), ())),
            precision=HIGHEST,
            preferred_element_type=jnp.float32,
        )
        decay, weights, updates, readings = None, [], [], []
        for t in range(NEW):
            beta = aux[t : t + 1, head : head + 1]
            keep = aux[t : t + 1, heads + head : heads + head + 1]
            recalled = first[t : t + 1] if t == 0 else decay * first[t : t + 1]
            for j in range(t):
                recalled = recalled + (weights[j] * pair[t : t + 1, j : j + 1]) * updates[j]
            updates.append(beta * (value[t : t + 1] - keep * recalled))
            decay = keep if t == 0 else decay * keep
            weights = [weight * keep for weight in weights] + [jnp.ones_like(keep)]
            reading = decay * first[NEW + t : NEW + t + 1]
            for j in range(t + 1):
                scaled = weights[j] * pair[NEW + t : NEW + t + 1, j : j + 1]
                reading = reading + scaled * updates[j]
            readings.append(reading)
        scaled_key = jnp.concatenate(
            [weights[j] * key[j : j + 1] for j in range(NEW)], axis=0
        )
        added = lax.dot_general(
            scaled_key,
            jnp.concatenate(updates, axis=0),
            (((0,), (0,)), ((), ())),
            precision=HIGHEST,
            preferred_element_type=jnp.float32,
        )
        next_ref[0, head] = decay * state + added
        reading = jnp.concatenate(readings, axis=0) * active
        normed = reading * lax.rsqrt(jnp.mean(reading * reading, axis=-1, keepdims=True) + EPS)
        normed = normed * gain * jax.nn.silu(gate_pre)
        mixed_ref[0, :, head * size : (head + 1) * size] = normed.astype(mixed_ref.dtype)


def run_delta(proj, aux, head_gain, state):
    seqs, heads, size, _ = state.shape
    by_seq = lambda *block: pl.BlockSpec(block, lambda s: (s,) + (0,) * (len(block) - 1))
    return pl.pallas_call(
        functools.partial(delta_kernel, heads),
        grid=(seqs,),
        in_specs=[
            by_seq(1, NEW, 4 * heads * size),
            by_seq(1, NEW, LANES),
            pl.BlockSpec((1, size), lambda s: (0, 0)),
            by_seq(1, heads, size, size),
        ],
        out_specs=[by_seq(1, NEW, heads * size), by_seq(1, heads, size, size)],
        out_shape=[
            jax.ShapeDtypeStruct((seqs, NEW, heads * size), jnp.bfloat16),
            jax.ShapeDtypeStruct(state.shape, jnp.float32),
        ],
        cost_estimate=pl.CostEstimate(
            flops=seqs * heads * size * size * 24,
            bytes_accessed=seqs * heads * size * size * 8,
            transcendentals=0,
        ),
    )(proj, aux, head_gain.reshape(1, size), state)


def split_square(squares):
    coarse = squares.astype(jnp.bfloat16)
    return coarse, (squares - coarse.astype(jnp.float32)).astype(jnp.bfloat16)


def pad_columns(columns):
    return jnp.pad(columns, ((0, 0), (0, -columns.shape[1] % LANES)))


def fast_split(size):
    return 1 << ((size.bit_length() - 1) // 2)


def scatter_two_stages(rows, axis):
    size, me = lax.axis_size(axis), lax.axis_index(axis)
    near = fast_split(size)
    count = rows.shape[0] // size
    total = None
    for far in [d for d in far_first(size) if d % near == 0] + [0]:
        terms = [block_of(rows, me ^ far, count)]
        for d in range(1, near):
            terms.append(swap(block_of(rows, me ^ far ^ d, count), axis, d))
        part = add_up(terms)
        if far:
            part = swap(part.astype(jnp.bfloat16), axis, far).astype(jnp.float32)
        total = part if total is None else total + part
    return total


def local(
    layer_input,
    seq_lengths,
    delta_state,
    attn_gain,
    w_query,
    w_key,
    w_value,
    w_outgate,
    w_write,
    w_forget,
    forget_rate,
    head_gain,
    w_out,
    mixer_gain,
    w_gate,
    w_up,
    w_down,
):
    feature_part = layer_input.shape[1]
    feature_anchor = lax.axis_index("kv") * feature_part
    seqs_here, heads_here = delta_state.shape[:2]
    head_size = head_gain.shape[0]
    wide = heads_here * head_size
    gathered = lax.all_gather(layer_input, "tp", axis=0, tiled=True)
    rows_wide = gathered.astype(jnp.float32)
    squares = jnp.sum(rows_wide * rows_wide, axis=1, keepdims=True)
    gain_part = lax.dynamic_slice_in_dim(attn_gain, feature_anchor, feature_part)
    normed_in = (rows_wide * gain_part.astype(jnp.float32)).astype(jnp.bfloat16)
    parts = [
        jnp.dot(normed_in, weight, preferred_element_type=jnp.float32).astype(jnp.bfloat16)
        for weight in (
            w_query, w_key, w_value, w_outgate, jnp.concatenate([w_write, w_forget], axis=1)
        )
    ]
    small = pad_columns(jnp.concatenate([parts[4], *split_square(squares)], axis=1))
    summed = add_up(scatter_blocks(jnp.concatenate(parts[:4] + [small], axis=1), "kv"))
    rest = summed[:, 4 * wide :]
    own_squares = rest[:, 2 * heads_here : 2 * heads_here + 1]
    own_squares = own_squares + rest[:, 2 * heads_here + 1 : 2 * heads_here + 2]
    row_scale = lax.rsqrt(own_squares / D + EPS)
    proj = (summed[:, : 4 * wide] * row_scale).reshape(seqs_here, NEW, 4 * wide)
    rates = (rest[:, : 2 * heads_here] * row_scale).reshape(seqs_here, NEW, 2 * heads_here)
    positions = jnp.arange(NEW, dtype=jnp.int32)
    live = (positions[None, :] < seq_lengths[:, None]).astype(jnp.float32)[:, :, None]
    beta = jax.nn.sigmoid(rates[:, :, :heads_here]) * live
    keep = jnp.exp(-forget_rate * jax.nn.softplus(rates[:, :, heads_here:]) * live)
    aux = jnp.concatenate([beta, keep, live], axis=2)
    aux = jnp.pad(aux, ((0, 0), (0, 0), (0, LANES - aux.shape[2])))
    mixed, carried = run_delta(proj, aux, head_gain, delta_state)
    mixed = mixed.reshape(seqs_here * NEW, wide)
    out_terms = gathered_dot(gather_blocks(mixed, "kv"), w_out, "kv")
    attended = add_up(scatter_blocks(out_terms, "tp"))
    hidden_state = (layer_input.astype(jnp.float32) + attended).astype(jnp.bfloat16)
    hidden_rows = lax.all_gather(hidden_state, "tp", axis=0, tiled=True)
    hidden_wide = hidden_rows.astype(jnp.float32)
    mixer_squares = jnp.sum(hidden_wide * hidden_wide, axis=1, keepdims=True)
    mixer_part = lax.dynamic_slice_in_dim(mixer_gain, feature_anchor, feature_part)
    normed_mid = (hidden_wide * mixer_part.astype(jnp.float32)).astype(jnp.bfloat16)
    gate_terms = jnp.dot(normed_mid, w_gate, preferred_element_type=jnp.float32)
    up_terms = jnp.dot(normed_mid, w_up, preferred_element_type=jnp.float32)
    units = w_gate.shape[1]
    small = pad_columns(jnp.concatenate(split_square(mixer_squares), axis=1))
    sums = scatter_two_stages(
        jnp.concatenate(
            [gate_terms.astype(jnp.bfloat16), up_terms.astype(jnp.bfloat16), small], axis=1
        ),
        "kv",
    )
    square_rows = sums[:, 2 * units : 2 * units + 1] + sums[:, 2 * units + 1 : 2 * units + 2]
    mixer_scale = lax.rsqrt(square_rows / D + EPS)
    activated = jax.nn.silu(mixer_scale * sums[:, :units])
    activated = (activated * (mixer_scale * sums[:, units : 2 * units])).astype(jnp.bfloat16)
    mixer_terms = gathered_dot(gather_blocks(activated, "kv"), w_down, "kv")
    mixer_out = add_up(scatter_blocks(mixer_terms, "tp"))
    layer_output = (hidden_state.astype(jnp.float32) + mixer_out).astype(jnp.bfloat16)
    return (layer_output, carried)


def solution(mesh):
    in_specs = (
        P("tp", "kv"),
        P("kv"),
        P("kv", "tp", None, None),
        P(),
        P("kv", "tp"),
        P("kv", "tp"),
        P("kv", "tp"),
        P("kv", "tp"),
        P("kv", "tp"),
        P("kv", "tp"),
        P("tp"),
        P(),
        P("tp", "kv"),
        P(),
        P("kv", "tp"),
        P("kv", "tp"),
        P("tp", "kv"),
    )
    out_specs = (P("tp", "kv"), P("kv", "tp", None, None))
    return jax.shard_map(local, mesh=mesh, in_specs=in_specs, out_specs=out_specs, check_vma=False)
```

```python
import functools

import jax
import jax.numpy as jnp
from jax import lax
from jax.experimental import pallas as pl
from jax.experimental.pallas import tpu as pltpu
from jax.sharding import PartitionSpec as P

D = 4096
NEW = 4
EPS = 1e-06
LANES = 128
HIGHEST = lax.Precision.HIGHEST


def swap(block, axis, distance):
    size = lax.axis_size(axis)
    return lax.ppermute(block, axis, [(i, i ^ distance) for i in range(size)])


def far_first(size):
    return sorted(range(1, size), key=lambda d: -d)


def fast_split(size):
    return 1 << ((size.bit_length() - 1) // 2)


def far_distances(size):
    near = fast_split(size)
    return [d for d in far_first(size) if d % near == 0]


def block_of(rows, index, count):
    return lax.dynamic_slice_in_dim(rows, index * count, count)


def scatter_blocks(rows, axis):
    size, me = lax.axis_size(axis), lax.axis_index(axis)
    count = rows.shape[0] // size
    got = [swap(block_of(rows, me ^ d, count), axis, d) for d in far_first(size)]
    return [block_of(rows, me, count)] + got


def add_up(terms):
    total = terms[0].astype(jnp.float32)
    for term in terms[1:]:
        total = total + term.astype(jnp.float32)
    return total


def gather_blocks(block, axis, name):
    size = lax.axis_size(axis)
    near = fast_split(size)
    blocks = {0: block}
    for far in far_distances(size):
        with jax.named_scope(f"{name}_far{far}"):
            blocks[far] = swap(block, axis, far)
    for far in [0] + far_distances(size)[::-1]:
        for d in range(1, near):
            with jax.named_scope(f"{name}_near{far}"):
                blocks[far + d] = swap(blocks[far], axis, d)
    return blocks


def gathered_dot_kernel(distances, me_ref, *refs):
    blocks, (weight_ref, out_ref, rows_ref) = refs[: len(distances)], refs[len(distances) :]
    count = blocks[0].shape[0]
    me = me_ref[0]
    for distance, block in zip(distances, blocks):
        start = pl.multiple_of((me ^ distance) * count, count)
        rows_ref[pl.ds(start, count), :] = block[...]
    out_ref[...] = jnp.dot(
        rows_ref[...], weight_ref[...], preferred_element_type=jnp.float32
    ).astype(out_ref.dtype)


def gathered_dot(pieces, weight, axis):
    distances = tuple(pieces)
    count, depth = pieces[0].shape
    rows, width = count * len(distances), weight.shape[1]
    me = lax.axis_index(axis).astype(jnp.int32).reshape(1)
    in_vmem = pl.BlockSpec(memory_space=pltpu.VMEM)
    return pl.pallas_call(
        functools.partial(gathered_dot_kernel, distances),
        out_shape=jax.ShapeDtypeStruct((rows, width), jnp.bfloat16),
        in_specs=[pl.BlockSpec(memory_space=pltpu.SMEM)] + [in_vmem] * (len(distances) + 1),
        out_specs=in_vmem,
        scratch_shapes=[pltpu.VMEM((rows, depth), jnp.bfloat16)],
        compiler_params=pltpu.CompilerParams(vmem_limit_bytes=16 * 1024 * 1024),
        cost_estimate=pl.CostEstimate(
            flops=2 * rows * depth * width, bytes_accessed=2 * depth * width, transcendentals=0
        ),
    )(me, *[pieces[d] for d in distances], weight)


def unit_norm(vectors):
    return vectors * lax.rsqrt(jnp.sum(vectors * vectors, axis=-1, keepdims=True) + EPS)


def delta_kernel(proj_ref, aux_ref, gain_ref, state_ref, mixed_ref, next_ref, *scratch):
    both_ref, first_ref, scaled_ref, update_ref, decay_ref = scratch
    count, size = proj_ref.shape[2:]
    pack = 2 * NEW
    gain = gain_ref[...]

    def slot(t):
        return pl.ds(t, count, stride=pack)

    keys, queries, values = [], [], []
    for t in range(NEW):
        queries.append(unit_norm(jax.nn.silu(proj_ref[0, t])) * size ** (-0.5))
        keys.append(unit_norm(jax.nn.silu(proj_ref[1, t])))
        values.append(jax.nn.silu(proj_ref[2, t]))
        both_ref[slot(t), :] = keys[t]
        both_ref[slot(NEW + t), :] = queries[t]
    for i in range(count):
        first_ref[i * pack : (i + 1) * pack, :] = jnp.dot(
            both_ref[i * pack : (i + 1) * pack, :],
            state_ref[i],
            precision=HIGHEST,
            preferred_element_type=jnp.float32,
        )

    def inner(left, right):
        return jnp.sum(left * right, axis=-1, keepdims=True)

    decay, weights, updates = None, [], []
    for t in range(NEW):
        aux = aux_ref[t]
        beta, keep, active = aux[:, 0:1], aux[:, 1:2], aux[:, 2:3]
        recalled = first_ref[slot(t), :]
        if t:
            recalled = decay * recalled
        for j in range(t):
            recalled = recalled + (weights[j] * inner(keys[t], keys[j])) * updates[j]
        updates.append(beta * (values[t] - keep * recalled))
        decay = keep if t == 0 else decay * keep
        weights = [weight * keep for weight in weights] + [jnp.ones_like(keep)]
        reading = decay * first_ref[slot(NEW + t), :]
        for j in range(t + 1):
            reading = reading + (weights[j] * inner(queries[t], keys[j])) * updates[j]
        reading = reading * active
        normed = reading * lax.rsqrt(jnp.mean(reading * reading, axis=-1, keepdims=True) + EPS)
        normed = normed * gain * jax.nn.silu(proj_ref[3, t])
        mixed_ref[t] = normed.astype(mixed_ref.dtype)
    for t in range(NEW):
        scaled_ref[slot(t), :] = weights[t] * keys[t]
        update_ref[slot(t), :] = updates[t]
        scaled_ref[slot(NEW + t), :] = jnp.zeros_like(keys[t])
        update_ref[slot(NEW + t), :] = jnp.zeros_like(keys[t])
    decay_ref[...] = jnp.broadcast_to(decay, decay_ref.shape)
    for i in range(count):
        added = lax.dot_general(
            scaled_ref[i * pack : (i + 1) * pack, :],
            update_ref[i * pack : (i + 1) * pack, :],
            (((0,), (0,)), ((), ())),
            precision=HIGHEST,
            preferred_element_type=jnp.float32,
        )
        next_ref[i] = decay_ref[i : i + 1, :] * state_ref[i] + added


def run_delta(proj, aux, head_gain, state):
    count, size = proj.shape[2:]
    in_vmem = pl.BlockSpec(memory_space=pltpu.VMEM)
    packed = pltpu.VMEM((count * 2 * NEW, size), jnp.float32)
    mixed, carried = pl.pallas_call(
        delta_kernel,
        in_specs=[in_vmem] * 4,
        out_specs=[in_vmem] * 2,
        out_shape=[
            jax.ShapeDtypeStruct((NEW, count, size), jnp.bfloat16),
            jax.ShapeDtypeStruct((count, size, size), jnp.float32),
        ],
        scratch_shapes=[packed] * 4 + [pltpu.VMEM((count, size), jnp.float32)],
        compiler_params=pltpu.CompilerParams(vmem_limit_bytes=16 * 1024 * 1024),
        cost_estimate=pl.CostEstimate(
            flops=count * size * size * 24,
            bytes_accessed=count * size * size * 8,
            transcendentals=0,
        ),
    )(proj, aux, head_gain.reshape(1, size), state.reshape(count, size, size))
    return mixed, carried.reshape(state.shape)


def split_square(squares):
    coarse = squares.astype(jnp.bfloat16)
    return coarse, (squares - coarse.astype(jnp.float32)).astype(jnp.bfloat16)


def pad_columns(columns):
    return jnp.pad(columns, ((0, 0), (0, -columns.shape[1] % LANES)))


def stage_order(size):
    fars = far_distances(size)
    middle = [d for d in fars if 2 * d >= size]
    return middle[::-1] + [d for d in fars if 2 * d < size] + [0]


def scatter_two_stages(rows, axis, name):
    size, me = lax.axis_size(axis), lax.axis_index(axis)
    near = fast_split(size)
    count = rows.shape[0] // size
    total, sums = None, []
    for far in stage_order(size):
        own = block_of(rows, me ^ far, count)
        if sums:
            own, sums[-1] = lax.optimization_barrier((own, sums[-1]))
        terms = [own]
        for d in range(1, near):
            other = block_of(rows, me ^ far ^ d, count)
            if len(sums) > 1:
                other, sums[-2] = lax.optimization_barrier((other, sums[-2]))
            with jax.named_scope(f"{name}_near{far}"):
                terms.append(swap(other, axis, d))
        part = add_up(terms)
        if far:
            part = part.astype(jnp.bfloat16)
            sums.append(part)
            with jax.named_scope(f"{name}_far{far}"):
                part = swap(part, axis, far)
            part = part.astype(jnp.float32)
        total = part if total is None else total + part
    return total


def local(
    layer_input,
    seq_lengths,
    delta_state,
    attn_gain,
    w_query,
    w_key,
    w_value,
    w_outgate,
    w_write,
    w_forget,
    forget_rate,
    head_gain,
    w_out,
    mixer_gain,
    w_gate,
    w_up,
    w_down,
):
    feature_part = layer_input.shape[1]
    feature_anchor = lax.axis_index("kv") * feature_part
    seqs_here, heads_here = delta_state.shape[:2]
    head_size = head_gain.shape[0]
    wide = heads_here * head_size
    gathered = lax.all_gather(layer_input, "tp", axis=0, tiled=True)
    rows_wide = gathered.astype(jnp.float32)
    squares = jnp.sum(rows_wide * rows_wide, axis=1, keepdims=True)
    gain_part = lax.dynamic_slice_in_dim(attn_gain, feature_anchor, feature_part)
    normed_in = (rows_wide * gain_part.astype(jnp.float32)).astype(jnp.bfloat16)
    parts = [
        jnp.dot(normed_in, weight, preferred_element_type=jnp.float32).astype(jnp.bfloat16)
        for weight in (
            w_query, w_key, w_value, w_outgate, jnp.concatenate([w_write, w_forget], axis=1)
        )
    ]
    small = pad_columns(jnp.concatenate([parts[4], *split_square(squares)], axis=1))
    summed = add_up(scatter_blocks(jnp.concatenate(parts[:4] + [small], axis=1), "kv"))
    rest = summed[:, 4 * wide :]
    own_squares = rest[:, 2 * heads_here : 2 * heads_here + 1]
    own_squares = own_squares + rest[:, 2 * heads_here + 1 : 2 * heads_here + 2]
    row_scale = lax.rsqrt(own_squares / D + EPS)
    proj = (summed[:, : 4 * wide] * row_scale).reshape(
        seqs_here, NEW, 4, heads_here, head_size
    )
    proj = proj.transpose(2, 1, 0, 3, 4).reshape(4, NEW, seqs_here * heads_here, head_size)
    rates = (rest[:, : 2 * heads_here] * row_scale).reshape(seqs_here, NEW, 2 * heads_here)
    positions = jnp.arange(NEW, dtype=jnp.int32)
    live = (positions[None, :] < seq_lengths[:, None]).astype(jnp.float32)[:, :, None]
    beta = jax.nn.sigmoid(rates[:, :, :heads_here]) * live
    keep = jnp.exp(-forget_rate * jax.nn.softplus(rates[:, :, heads_here:]) * live)
    aux = jnp.stack([beta, keep, jnp.broadcast_to(live, beta.shape)], axis=-1)
    aux = aux.transpose(1, 0, 2, 3).reshape(NEW, seqs_here * heads_here, 3)
    mixed, carried = run_delta(proj, aux, head_gain, delta_state)
    mixed = mixed.reshape(NEW, seqs_here, heads_here, head_size).transpose(1, 0, 2, 3)
    mixed = mixed.reshape(seqs_here * NEW, wide)
    out_terms = gathered_dot(gather_blocks(mixed, "kv", "heads"), w_out, "kv")
    attended = add_up(scatter_blocks(out_terms, "tp"))
    hidden_state = (layer_input.astype(jnp.float32) + attended).astype(jnp.bfloat16)
    hidden_rows = lax.all_gather(hidden_state, "tp", axis=0, tiled=True)
    hidden_wide = hidden_rows.astype(jnp.float32)
    mixer_squares = jnp.sum(hidden_wide * hidden_wide, axis=1, keepdims=True)
    mixer_part = lax.dynamic_slice_in_dim(mixer_gain, feature_anchor, feature_part)
    normed_mid = (hidden_wide * mixer_part.astype(jnp.float32)).astype(jnp.bfloat16)
    gate_terms = jnp.dot(normed_mid, w_gate, preferred_element_type=jnp.float32)
    up_terms = jnp.dot(normed_mid, w_up, preferred_element_type=jnp.float32)
    units = w_gate.shape[1]
    small = pad_columns(jnp.concatenate(split_square(mixer_squares), axis=1))
    sums = scatter_two_stages(
        jnp.concatenate(
            [gate_terms.astype(jnp.bfloat16), up_terms.astype(jnp.bfloat16), small], axis=1
        ),
        "kv",
        "mixer",
    )
    square_rows = sums[:, 2 * units : 2 * units + 1] + sums[:, 2 * units + 1 : 2 * units + 2]
    mixer_scale = lax.rsqrt(square_rows / D + EPS)
    activated = jax.nn.silu(mixer_scale * sums[:, :units])
    activated = (activated * (mixer_scale * sums[:, units : 2 * units])).astype(jnp.bfloat16)
    mixer_terms = gathered_dot(gather_blocks(activated, "kv", "units"), w_down, "kv")
    mixer_out = add_up(scatter_blocks(mixer_terms, "tp"))
    layer_output = (hidden_state.astype(jnp.float32) + mixer_out).astype(jnp.bfloat16)
    return (layer_output, carried)


def solution(mesh):
    in_specs = (
        P("tp", "kv"),
        P("kv"),
        P("kv", "tp", None, None),
        P(),
        P("kv", "tp"),
        P("kv", "tp"),
        P("kv", "tp"),
        P("kv", "tp"),
        P("kv", "tp"),
        P("kv", "tp"),
        P("tp"),
        P(),
        P("tp", "kv"),
        P(),
        P("kv", "tp"),
        P("kv", "tp"),
        P("tp", "kv"),
    )
    out_specs = (P("tp", "kv"), P("kv", "tp", None, None))
    return jax.shard_map(local, mesh=mesh, in_specs=in_specs, out_specs=out_specs, check_vma=False)
```
